256 devices in a mesh: grp: 2 (over y), kv: 16 (over z), tp: 8 (over x, core).
Axes of the slice: x: 4, y: 2, z: 16, core: 2. Of those that a mesh axis runs over, the one named last changes fastest.
The devices are a block of a 4x16x16 slice.
Arguments:
- tokens: bfloat16 [512, 2048], P('grp', 'kv'), parts along dimension 0, may hold values from -64 to 64
- lengths: int32 [512], P(('grp', 'kv')), parts along dimension 0, may hold values from 1 to 4096, 131072 in all
- state: float32 [512, 8, 128, 256], P(('grp', 'kv'), 'tp'), parts along dimension 0, may hold values from -6 to 6
- key_block: bfloat16 [512, 8, 64, 128], P(('grp', 'kv'), 'tp'), parts along dimension 0, may hold values from -6 to 6
- value_block: bfloat16 [512, 8, 64, 256], P(('grp', 'kv'), 'tp'), parts along dimension 0, may hold values from -6 to 6
- cum_decay: float32 [512, 8, 64, 128], P(('grp', 'kv'), 'tp'), parts along dimension 0, as said below
- step_decay: float32 [512, 1024], P(('grp', 'kv'), 'tp'), parts along dimension 0
- g_mix: bfloat16 [2048], P('kv'), may hold values from 0.099609375 to 1.8984375
- w_query: bfloat16 [2048, 1024], P('kv', 'tp'), may hold values from -0.125 to 0.125
- w_key: bfloat16 [2048, 1024], P('kv', 'tp'), may hold values from -0.125 to 0.125
- w_value: bfloat16 [2048, 2048], P('kv', 'tp'), may hold values from -0.125 to 0.125
- w_outgate: bfloat16 [2048, 2048], P('kv', 'tp'), may hold values from -0.125 to 0.125
- w_decay: bfloat16 [2048, 1024], P('kv', 'tp'), may hold values from -0.5 to 0.5
- g_heads: bfloat16 [2048], P('tp'), may hold values from 0.099609375 to 1.8984375
- w_out: bfloat16 [2048, 2048], P('tp', 'kv'), may hold values from -0.125 to 0.125
- g_ffn: bfloat16 [2048], P('kv'), may hold values from 0.099609375 to 1.8984375
- w_gate: bfloat16 [2048, 5632], P('kv', 'tp'), may hold values from -0.125 to 0.125
- w_up: bfloat16 [2048, 5632], P('kv', 'tp'), may hold values from -0.125 to 0.125
- w_down: bfloat16 [5632, 2048], P('tp', 'kv'), may hold values from -0.078125 to 0.078125
Outputs:
- updated: bfloat16 [512, 2048], P('grp', 'kv'), parts along dimension 0
The draws below stay inside these ranges and needn't reach their ends.
There are 2 independent parts, one for each index of `grp`. The reference program is written for one: setup_inputs(seed, part) draws one part's arguments, and reference() takes and returns one part's arrays. A program takes and returns all parts, laid end to end along the dimension named above; an argument that names none is the same for every part. Nothing has to cross between parts.
Inputs may be any that keep to these rules, and one draw needn't show every extreme that they name: `cum_decay`: along the block's positions the entries never rise.
All inputs are finite; a program needn't handle non-finite values. No bound on the sum of `lengths` on one device may be relied on, other than what follows from the above.
Results may differ from the reference program's by a relative error of at most 0.019.
Values may be sent and summed in bfloat16 or wider, within the bound.
A program may use at most 64 MiB of HBM per device.

```python
import math
import jax
import jax.numpy as jnp
import numpy as np
from jax import lax

D = 2048
ATTN_GROUPS = 8
DK = 128
DV = 256
FF = 5632
SPAN_STEPS = 64
STREAM_NUMBER = 256
N_TP = 8


def head_rates(key):
    k_slow, k_fast, k_seq, k_chan = jax.random.split(key, 4)
    gradual_shrink_factor = jax.random.bernoulli(k_slow, 0.5, (1, ATTN_GROUPS, 1))
    fast_rate = jax.random.uniform(k_fast, (1, ATTN_GROUPS, 1), jnp.float32, 1.0 / 50.0, 1.0 / 30.0)
    slow_rate = jnp.float32(0.5 / SPAN_STEPS)
    seq_factor = jnp.exp(jax.random.uniform(k_seq, (STREAM_NUMBER, 1, 1), jnp.float32, math.log(0.5), math.log(2.0)))
    chan_factor = jax.random.uniform(k_chan, (1, ATTN_GROUPS, DK), jnp.float32, 0.5, 1.5)
    rate = jnp.where(gradual_shrink_factor, slow_rate, fast_rate) * seq_factor * chan_factor
    return (rate, gradual_shrink_factor)


def draw_tokens(key, part):
    k_base, k_rise, k_rows = jax.random.split(key, 3)
    columns = jnp.arange(D, dtype=jnp.float32) / D
    rough = jax.random.uniform(k_rise, (D,), jnp.float32, 0.5, 2.0)
    rows = jnp.exp(jax.random.uniform(k_rows, (STREAM_NUMBER, 1), jnp.float32, math.log(0.3), math.log(3.0)))
    base = jnp.clip(jax.random.normal(k_base, (STREAM_NUMBER, D), jnp.float32), -6.0, 6.0)
    rise = 3.0 ** columns * rough / 1.8
    return (base * rise[None, :] * rows).astype(jnp.bfloat16)


def draw_cum_decay(key, part):
    rate, gradual_shrink_factor = head_rates(jax.random.fold_in(key, 11))
    k_step, lookup_location, lookup_breadth = jax.random.split(jax.random.fold_in(key, 12), 3)
    steps = -rate[:, :, None, :] * jax.random.uniform(k_step, (STREAM_NUMBER, ATTN_GROUPS, SPAN_STEPS, DK), jnp.float32, 0.5, 1.5)
    span_offset = jax.random.randint(lookup_location, (STREAM_NUMBER, ATTN_GROUPS, 1, 2), 0, SPAN_STEPS)
    token_ordinal = jnp.arange(SPAN_STEPS, dtype=jnp.int32)[None, None, :, None]
    match_tally = jnp.any(token_ordinal == span_offset, axis=3)
    span_extent = jnp.log(jax.random.uniform(lookup_breadth, (STREAM_NUMBER, ATTN_GROUPS, 1), jnp.float32, 0.5, 0.8))
    surplus_tally = jnp.where(match_tally & gradual_shrink_factor, span_extent, jnp.float32(0.0))
    steps = steps + surplus_tally[:, :, :, None]
    return jnp.cumsum(steps, axis=2).astype(jnp.float32)


def draw_step_decay(key, part):
    rate, gradual_shrink_factor = head_rates(jax.random.fold_in(key, 11))
    k_step, lookup_location, lookup_breadth = jax.random.split(jax.random.fold_in(key, 13), 3)
    k_rough = jax.random.fold_in(key, 14)
    payload_element = -rate * jax.random.uniform(k_step, (STREAM_NUMBER, ATTN_GROUPS, DK), jnp.float32, 0.5, 1.5)
    payload_element = payload_element - jax.random.uniform(k_rough, (STREAM_NUMBER, ATTN_GROUPS, DK), jnp.float32, 0.0, 0.35)
    match_tally = jax.random.randint(lookup_location, (STREAM_NUMBER, ATTN_GROUPS, 1), 0, 2) == 0
    span_extent = jnp.log(jax.random.uniform(lookup_breadth, (STREAM_NUMBER, ATTN_GROUPS, 1), jnp.float32, 0.5, 0.8))
    payload_element = payload_element + jnp.where(match_tally & gradual_shrink_factor, span_extent, jnp.float32(0.0))
    return payload_element.reshape(STREAM_NUMBER, ATTN_GROUPS * DK).astype(jnp.float32)


def shard_levels(own_key, dims, shards, low, largest):
    level, own = 1.0, jax.random.fold_in(own_key, 6)
    for position, shards_of in shards:
        heights = jnp.exp(jax.random.uniform(jax.random.fold_in(own, position), (shards_of,), jnp.float32, low / len(shards), largest / len(shards)))
        level = level * jnp.repeat(heights, dims[position] // shards_of).reshape([-1 if axis == position else 1 for axis in range(len(dims))])
    return level


def length_profile(count, total, limit, skew):
    weights = [(1 << 20) // math.isqrt(grade ** skew) + 1 for grade in range(2, count + 1)]
    rest, given = total - limit - (count - 1), [1] * (count - 1)
    while rest > 0:
        movable = [i for i in range(count - 1) if given[i] < limit]
        mass, left = sum([weights[i] for i in movable]), rest
        for i in movable:
            extra = min(limit - given[i], max(1, left * weights[i] // mass), rest)
            given[i] = given[i] + extra
            rest = rest - extra
    return np.array([limit] + given)


def uneven_parts(own_key, amount, total, limit, lean):
    if amount == 2:
        one = jax.random.randint(own_key, (), max(1, total - limit), min(limit, total - 1) + 1)
        return jnp.stack([one, total - one])
    sizes = jnp.asarray(length_profile(amount, total, limit, lean), jnp.int32)
    twos = (amount - 1) // 2
    source_of, receiver = sizes[1:1 + 2 * twos:2], sizes[2:2 + 2 * twos:2]
    slack = jnp.minimum(source_of - 1, limit - receiver)
    moved = jax.random.randint(jax.random.fold_in(own_key, 1), (twos,), 0, 1 << 20) % (slack + 1)
    sizes = sizes.at[1:1 + 2 * twos:2].set(source_of - moved).at[2:2 + 2 * twos:2].set(receiver + moved)
    return sizes[jax.random.permutation(jax.random.fold_in(own_key, 2), amount)]


def gaussian(key, extent, scale, most, cuts=(), kind=jnp.bfloat16):
    factor_of = shard_levels(key, extent, cuts, -0.22, 0.18) if cuts else 1.0
    entries = jax.random.normal(key, extent, jnp.float32) * scale * factor_of
    return jnp.minimum(jnp.maximum(entries, -most), most).astype(kind)


def setup_inputs(seed: int = 0, part: int = 0) -> dict:
    streams_of = jax.random.split(jax.random.key(seed), 20)
    part_splits = jax.random.split(jax.random.fold_in(streams_of[19], part), 20)
    return {
        "tokens": draw_tokens(jax.random.fold_in(jax.random.fold_in(streams_of[19], part), 71), part),
        "lengths": uneven_parts(part_splits[1], STREAM_NUMBER, STREAM_NUMBER * 512, min(4096, STREAM_NUMBER * 256), 2).astype(jnp.int32),
        "state": gaussian(part_splits[2], (STREAM_NUMBER, ATTN_GROUPS, DK, DV), 1.0, 6.0, ((0, 16), (1, 8)), jnp.float32),
        "key_block": gaussian(part_splits[3], (STREAM_NUMBER, ATTN_GROUPS, SPAN_STEPS, DK), 1.0, 6.0, ((0, 16), (1, 8))),
        "value_block": gaussian(part_splits[4], (STREAM_NUMBER, ATTN_GROUPS, SPAN_STEPS, DV), 1.0, 6.0, ((0, 16), (1, 8))),
        "cum_decay": draw_cum_decay(jax.random.fold_in(jax.random.fold_in(streams_of[19], part), 71), part),
        "step_decay": draw_step_decay(jax.random.fold_in(jax.random.fold_in(streams_of[19], part), 71), part),
        "g_mix": jnp.clip(1.0 + 0.18 * jax.random.normal(streams_of[7], (D,), jnp.float32), 0.099609375, 1.8984375).astype(jnp.bfloat16),
        "w_query": gaussian(streams_of[8], (D, ATTN_GROUPS * DK), D ** -0.5, 0.125, ((0, 16), (1, 8))),
        "w_key": gaussian(streams_of[9], (D, ATTN_GROUPS * DK), D ** -0.5, 0.125, ((0, 16), (1, 8))),
        "w_value": gaussian(streams_of[10], (D, ATTN_GROUPS * DV), D ** -0.5, 0.125, ((0, 16), (1, 8))),
        "w_outgate": gaussian(streams_of[11], (D, ATTN_GROUPS * DV), D ** -0.5, 0.125, ((0, 16), (1, 8))),
        "w_decay": gaussian(streams_of[12], (D, ATTN_GROUPS * DK), (D // 16) ** -0.5, 0.5, ((0, 16), (1, 8))),
        "g_heads": jnp.clip(1.0 + 0.18 * jax.random.normal(streams_of[13], (ATTN_GROUPS * DV,), jnp.float32), 0.099609375, 1.8984375).astype(jnp.bfloat16),
        "w_out": gaussian(streams_of[14], (ATTN_GROUPS * DV, D), (ATTN_GROUPS * DV) ** -0.5, 0.125, ((0, 8), (1, 16))),
        "g_ffn": jnp.clip(1.0 + 0.18 * jax.random.normal(streams_of[15], (D,), jnp.float32), 0.099609375, 1.8984375).astype(jnp.bfloat16),
        "w_gate": gaussian(streams_of[16], (D, FF), D ** -0.5, 0.125, ((0, 16), (1, 8))),
        "w_up": gaussian(streams_of[17], (D, FF), D ** -0.5, 0.125, ((0, 16), (1, 8))),
        "w_down": gaussian(streams_of[18], (FF, D), FF ** -0.5, 0.078125, ((0, 8), (1, 16))),
    }


epsilon = 1e-06
temper = 16.0

def blocked_product(left, weight):
    block_rows = left.shape[1] // N_TP
    total = jnp.zeros((left.shape[0], weight.shape[1]), jnp.float32)
    for index in range(N_TP):
        part = jnp.dot(left[:, index * block_rows:(index + 1) * block_rows], weight[index * block_rows:(index + 1) * block_rows], preferred_element_type=jnp.float32)
        rounded = lax.optimization_barrier(part.astype(jnp.bfloat16))
        total = total + rounded.astype(jnp.float32)
    return total

def reference(tokens, lengths, state, key_block, value_block, cum_decay, step_decay, g_mix, w_query, w_key, w_value, w_outgate, w_decay, g_heads, w_out, g_ffn, w_gate, w_up, w_down):
    highest = lax.Precision.HIGHEST
    inputs = tokens.astype(jnp.float32)
    inverse = lax.rsqrt(lax.optimization_barrier(jnp.sum(inputs * inputs, axis=1)) / D + epsilon)[:, None]
    scaled = (inputs * g_mix.astype(jnp.float32)).astype(jnp.bfloat16)

    def project(matrix):
        return jnp.dot(scaled, matrix, preferred_element_type=jnp.float32) * inverse
    query = (project(w_query) * DK ** (-0.5)).reshape(STREAM_NUMBER, ATTN_GROUPS, DK)
    keys_new = project(w_key).reshape(STREAM_NUMBER, ATTN_GROUPS, DK)
    values_new = project(w_value).reshape(STREAM_NUMBER, ATTN_GROUPS, DV)
    out_gate = project(w_outgate)
    decay_pre = project(w_decay)
    log_step = (jax.nn.log_sigmoid(decay_pre) / temper + step_decay).reshape(STREAM_NUMBER, ATTN_GROUPS, DK)
    live_count = lengths % SPAN_STEPS
    token_ordinal = lax.broadcasted_iota(jnp.int32, (1, 1, SPAN_STEPS, 1), 2)
    picked = jnp.where(token_ordinal == live_count[:, None, None, None] - 1, cum_decay, jnp.float32(0.0))
    token_decay = lax.optimization_barrier(jnp.sum(picked, axis=2)) + log_step
    carried = jnp.einsum('shk,shkv->shv', query * jnp.exp(token_decay), state, precision=highest)
    scores = lax.optimization_barrier(jnp.sum(query[:, :, None, :] * key_block.astype(jnp.float32) * jnp.exp(token_decay[:, :, None, :] - cum_decay), axis=3))
    scores = jnp.where(token_ordinal[..., 0] < live_count[:, None, None], scores, jnp.float32(0.0))
    in_block = jnp.einsum('shj,shjv->shv', scores, value_block.astype(jnp.float32), precision=highest)
    own_term = lax.optimization_barrier(jnp.sum(query * keys_new, axis=2))[:, :, None] * values_new
    head_out = carried + in_block + own_term
    normed = head_out * lax.rsqrt(lax.optimization_barrier(jnp.mean(head_out * head_out, axis=2, keepdims=True)) + epsilon)
    normed = normed * g_heads.astype(jnp.float32).reshape(ATTN_GROUPS, DV)
    mixed = (normed.reshape(STREAM_NUMBER, ATTN_GROUPS * DV) * jax.nn.silu(out_gate)).astype(jnp.bfloat16)
    attention = blocked_product(mixed, w_out)
    residual = (inputs + attention).astype(jnp.bfloat16)
    middle = residual.astype(jnp.float32)
    mid_inverse = lax.rsqrt(lax.optimization_barrier(jnp.sum(middle * middle, axis=1)) / D + epsilon)[:, None]
    normed_mid = (middle * g_ffn.astype(jnp.float32)).astype(jnp.bfloat16)
    gate_sum = jnp.dot(normed_mid, w_gate, preferred_element_type=jnp.float32) * mid_inverse
    up_sum = jnp.dot(normed_mid, w_up, preferred_element_type=jnp.float32) * mid_inverse
    hidden = (jax.nn.silu(gate_sum) * up_sum).astype(jnp.bfloat16)
    return (middle + blocked_product(hidden, w_down)).astype(jnp.bfloat16)
```

```python
import functools

import jax
import jax.numpy as jnp
from jax import lax
from jax.experimental import pallas as pl
from jax.experimental.pallas import tpu as pltpu
from jax.sharding import PartitionSpec as P

D = 2048
DK = 128
DV = 256

epsilon = 1e-06
temper = 16.0

MESH = pl.DeviceIdType.MESH
LANES = 128
HUBS_PROJ = (3, 6)
HUBS_MIXED = (3, 6)
HUBS_FFN = (3, 6)
HUBS_HIDDEN = (3, 6)
f32 = jnp.float32
bf16 = jnp.bfloat16


class RingTree:
    def __init__(self, n, hubs):
        self.n = n
        self.far = (n // 2, n - 1 - n // 2)
        self.hubs = [[0] + [h for h in hubs if h < far] for far in self.far]

    def index(self, side, delta):
        return delta - 1 + side * self.far[0]

    def parent(self, side, delta):
        return max(h for h in self.hubs[side] if h < delta)

    def children(self, side, hub):
        return [d for d in range(1, self.far[side] + 1) if self.parent(side, d) == hub]

    def leaves(self, side, hub):
        return [d for d in self.children(side, hub) if d not in self.hubs[side]]

    def reach(self):
        return max(d - self.parent(s, d) for s in (0, 1) for d in range(1, self.far[s] + 1))

    def levels(self):
        return max(len(h) for h in self.hubs)


def ring_reduce_scatter(tree, me, part, slots, stage, send_sem, recv_sem):
    n = tree.n

    def node(offset):
        return lax.rem(me + (offset + n), n)

    def copy(side, delta, src):
        sign = 1 - 2 * side
        k = tree.index(side, delta)
        hop = delta - tree.parent(side, delta)
        return pltpu.make_async_remote_copy(
            src_ref=src,
            dst_ref=slots.at[k],
            send_sem=send_sem.at[k],
            recv_sem=recv_sem.at[k],
            device_id={"kv": node(-sign * hop)},
            device_id_type=MESH,
        )

    def owner(side, delta):
        return node(-(1 - 2 * side) * delta)

    started = []

    def send_leaves(level):
        todo = [
            [(s, d) for d in tree.leaves(s, tree.hubs[s][level])] if level < len(tree.hubs[s]) else []
            for s in (0, 1)
        ]
        for i in range(max(len(t) for t in todo)):
            for t in todo:
                if i < len(t):
                    side, delta = t[i]
                    c = copy(side, delta, part.at[owner(side, delta)])
                    c.start()
                    started.append(c)

    def combined(side, hub, own):
        total = own
        for delta in tree.children(side, hub):
            k = tree.index(side, delta)
            copy(side, delta, slots.at[k]).wait_recv()
            total = total + slots[k].astype(f32)
        return total

    top = tree.levels() - 1
    send_leaves(top)
    for level in range(top, 0, -1):
        send_leaves(level - 1)
        for side in (0, 1):
            if level < len(tree.hubs[side]):
                hub = tree.hubs[side][level]
                k = tree.index(side, hub)
                total = combined(side, hub, part[owner(side, hub)].astype(f32))
                spot = 2 * (level - 1) + side
                stage[spot] = total.astype(stage.dtype)
                c = copy(side, hub, stage.at[spot])
                c.start()
                started.append(c)
    total = part[me].astype(f32)
    for side in (0, 1):
        total = combined(side, 0, total)
    return total, started


def ring_all_gather(tree, me, whole, send_sem, recv_sem):
    n = tree.n

    def node(offset):
        return lax.rem(me + (offset + n), n)

    def copy(side, delta):
        sign = 1 - 2 * side
        k = tree.index(side, delta)
        hub = tree.parent(side, delta)
        block = whole.at[node(-sign * hub)]
        return pltpu.make_async_remote_copy(
            src_ref=block,
            dst_ref=block,
            send_sem=send_sem.at[k],
            recv_sem=recv_sem.at[k],
            device_id={"kv": node(sign * (delta - hub))},
            device_id_type=MESH,
        )

    def arrived(side, delta):
        sign = 1 - 2 * side
        k = tree.index(side, delta)
        block = whole.at[node(-sign * delta)]
        pltpu.make_async_remote_copy(
            src_ref=block,
            dst_ref=block,
            send_sem=send_sem.at[k],
            recv_sem=recv_sem.at[k],
            device_id={"kv": node(sign)},
            device_id_type=MESH,
        ).wait_recv()

    started = []
    waited = set()
    for level in range(tree.levels()):
        for side in (0, 1):
            if level < len(tree.hubs[side]):
                hub = tree.hubs[side][level]
                if hub:
                    arrived(side, hub)
                    waited.add((side, hub))
                for delta in reversed(tree.children(side, hub)):
                    c = copy(side, delta)
                    c.start()
                    started.append(c)
    for side in (0, 1):
        for delta in range(1, tree.far[side] + 1):
            if (side, delta) not in waited:
                arrived(side, delta)
    return started


def tp_exchange(n, me, block_for, slot_of, send_sem, recv_sem):
    copies = []
    for j in range(1, n):
        peer = lax.rem(me + j, n)
        copies.append(
            pltpu.make_async_remote_copy(
                src_ref=block_for(peer),
                dst_ref=slot_of(me, j),
                send_sem=send_sem.at[j],
                recv_sem=recv_sem.at[j],
                device_id={"tp": peer},
                device_id_type=MESH,
            )
        )
    for c in copies:
        c.start()
    return copies


def tp_arrived(n, me, slot_of, send_sem, recv_sem):
    for j in range(1, n):
        source = lax.rem(me + (n - j), n)
        slot = slot_of(source, j)
        pltpu.make_async_remote_copy(
            src_ref=slot,
            dst_ref=slot,
            send_sem=send_sem.at[j],
            recv_sem=recv_sem.at[j],
            device_id={"tp": source},
            device_id_type=MESH,
        ).wait_recv()


def tp_all_reduce(n, me, part, slots, whole, finish, send_sem, recv_sem):
    started = tp_exchange(n, me, lambda peer: part.at[peer], lambda source, j: slots.at[j], send_sem.at[0], recv_sem.at[0])
    tp_arrived(n, me, lambda source, j: slots.at[j], send_sem.at[0], recv_sem.at[0])
    total = part[me].astype(f32)
    for j in range(1, n):
        total = total + slots[j].astype(f32)
    whole[me] = finish(total).astype(whole.dtype)
    started += tp_exchange(n, me, lambda peer: whole.at[me], lambda source, j: whole.at[source], send_sem.at[1], recv_sem.at[1])
    tp_arrived(n, me, lambda source, j: whole.at[source], send_sem.at[1], recv_sem.at[1])
    return started


def silu(v):
    return v / (1.0 + jnp.exp(-v))


def kernel(n_kv, n_tp, trees, names, *refs):
    count = len(names)
    hbm = dict(zip(names, refs[:count]))
    lengths = refs[count]
    out = refs[count + 1]
    vm = dict(zip(names, refs[count + 2 : 2 * count + 2]))
    (
        load_sem,
        part_a,
        slots_a,
        stage_a,
        mixed_all,
        part_c,
        slots_c,
        res_all,
        part_d,
        slots_d,
        stage_d,
        hidden_all,
        part_f,
        slots_f,
        out_all,
        send_a,
        recv_a,
        send_b,
        recv_b,
        send_c,
        recv_c,
        send_d,
        recv_d,
        send_e,
        recv_e,
        send_f,
        recv_f,
    ) = refs[2 * count + 2 :]
    kv = lax.axis_index("kv")
    tp = lax.axis_index("tp")
    tree_a, tree_b, tree_d, tree_e = trees

    reach = max(t.reach() for t in trees)
    barrier = pltpu.get_barrier_semaphore()
    peers = 0
    for o in range(1, reach + 1):
        for offset in (o, n_kv - o):
            pl.semaphore_signal(
                barrier, inc=1, device_id={"kv": lax.rem(kv + offset, n_kv)}, device_id_type=MESH
            )
            peers += 1
    for j in range(1, n_tp):
        pl.semaphore_signal(barrier, inc=1, device_id={"tp": lax.rem(tp + j, n_tp)}, device_id_type=MESH)
        peers += 1

    loads = {}
    for i, name in enumerate(names):
        loads[name] = pltpu.make_async_copy(hbm[name], vm[name], load_sem.at[i])
        loads[name].start()

    for name in ("tokens", "g_mix", "w_query", "w_key", "w_value", "w_outgate", "w_decay"):
        loads[name].wait()
    seqs = part_a.shape[1]
    inputs = vm["tokens"][...].astype(f32)
    rows = inputs.shape[0]
    scaled = (inputs * vm["g_mix"][...].astype(f32)).astype(bf16)
    at = 0
    for name in ("w_query", "w_key", "w_value", "w_outgate", "w_decay"):
        weight = vm[name][...]
        width = weight.shape[1]
        product = jnp.dot(scaled, weight, preferred_element_type=f32)
        part_a[:, :, at : at + width] = product.astype(bf16).reshape(n_kv, seqs, width)
        at += width
    square = jnp.broadcast_to(jnp.sum(inputs * inputs, axis=1, keepdims=True), (rows, LANES))
    part_a[:, :, at : at + LANES] = square.astype(bf16).reshape(n_kv, seqs, LANES)

    pl.semaphore_wait(barrier, peers)
    projected, started = ring_reduce_scatter(tree_a, kv, part_a, slots_a, stage_a, send_a, recv_a)

    for name in names:
        if name not in ("tokens", "g_mix", "w_query", "w_key", "w_value", "w_outgate", "w_decay"):
            loads[name].wait()

    inverse = lax.rsqrt(projected[:, at : at + 1] / D + epsilon)
    projected = projected * inverse
    query = projected[:, :DK] * DK ** (-0.5)
    keys_new = projected[:, DK : 2 * DK]
    values_new = projected[:, 2 * DK : 2 * DK + DV]
    out_gate = projected[:, 2 * DK + DV : 2 * DK + 2 * DV]
    decay_pre = projected[:, 2 * DK + 2 * DV : 3 * DK + 2 * DV]
    log_sig = jnp.minimum(decay_pre, 0.0) - jnp.log1p(jnp.exp(-jnp.abs(decay_pre)))
    log_step = log_sig / temper + vm["step_decay"][...]

    block_len = vm["key_block"].shape[2]
    ordinal = lax.broadcasted_iota(jnp.int32, (block_len, DK), 0)
    ordinal_column = lax.broadcasted_iota(jnp.int32, (block_len, 1), 0)
    live = [lax.rem(lengths[s], block_len) for s in range(seqs)]
    picked = [
        jnp.sum(
            jnp.where(ordinal == live[s] - 1, vm["cum_decay"][s, 0], 0.0), axis=0, keepdims=True
        )
        for s in range(seqs)
    ]
    token_decay = jnp.concatenate(picked, axis=0) + log_step
    weighted = jnp.transpose(query * jnp.exp(token_decay))
    heads_out = []
    for s in range(seqs):
        carried = jnp.sum(weighted[:, s : s + 1] * vm["state"][s, 0], axis=0, keepdims=True)
        scores = jnp.sum(
            query[s : s + 1]
            * vm["key_block"][s, 0].astype(f32)
            * jnp.exp(token_decay[s : s + 1] - vm["cum_decay"][s, 0]),
            axis=1,
            keepdims=True,
        )
        scores = jnp.where(ordinal_column < live[s], scores, 0.0)
        in_block = jnp.sum(scores * vm["value_block"][s, 0].astype(f32), axis=0, keepdims=True)
        heads_out.append(carried + in_block)
    head_out = jnp.concatenate(heads_out, axis=0)
    head_out = head_out + jnp.sum(query * keys_new, axis=1, keepdims=True) * values_new
    normed = head_out * lax.rsqrt(jnp.mean(head_out * head_out, axis=1, keepdims=True) + epsilon)
    normed = normed * vm["g_heads"][...].astype(f32)
    mixed_all[kv] = (normed * silu(out_gate)).astype(bf16)

    started += ring_all_gather(tree_b, kv, mixed_all, send_b, recv_b)
    attn_part = jnp.dot(
        mixed_all[...].reshape(rows, DV), vm["w_out"][...], preferred_element_type=f32
    ).astype(bf16)
    width = part_c.shape[2]
    piece = rows // n_tp
    part_c[...] = attn_part.reshape(n_tp, piece, width)
    own_rows = pl.ds(pl.multiple_of(tp * piece, piece), piece)

    started += tp_all_reduce(
        n_tp,
        tp,
        part_c,
        slots_c,
        res_all,
        lambda total: vm["tokens"][own_rows].astype(f32) + total,
        send_c,
        recv_c,
    )
    middle = res_all[...].reshape(rows, width).astype(f32)
    normed_mid = (middle * vm["g_ffn"][...].astype(f32)).astype(bf16)
    units = vm["w_gate"].shape[1]
    padded = part_d.shape[2] // 2
    square_mid = jnp.sum(middle * middle, axis=1, keepdims=True)
    gate_part = jnp.dot(normed_mid, vm["w_gate"][...], preferred_element_type=f32)
    part_d[:, :, :units] = gate_part.astype(bf16).reshape(n_kv, seqs, units)
    rest = padded - units
    part_d[:, :, units:padded] = (
        jnp.broadcast_to(square_mid, (rows, rest)).astype(bf16).reshape(n_kv, seqs, rest)
    )
    up_part = jnp.dot(normed_mid, vm["w_up"][...], preferred_element_type=f32)
    part_d[:, :, padded : padded + units] = up_part.astype(bf16).reshape(n_kv, seqs, units)

    total, sent = ring_reduce_scatter(tree_d, kv, part_d, slots_d, stage_d, send_d, recv_d)
    started += sent
    mid_inverse = lax.rsqrt(total[:, units : units + 1] / D + epsilon)
    gate_sum = total[:, :units] * mid_inverse
    up_sum = total[:, padded : padded + units] * mid_inverse
    hidden_all[kv] = (silu(gate_sum) * up_sum).astype(bf16)

    started += ring_all_gather(tree_e, kv, hidden_all, send_e, recv_e)
    down_part = jnp.dot(
        hidden_all[...].reshape(rows, units), vm["w_down"][...], preferred_element_type=f32
    ).astype(bf16)
    part_f[...] = down_part.reshape(n_tp, piece, width)
    started += tp_all_reduce(
        n_tp,
        tp,
        part_f,
        slots_f,
        out_all,
        lambda total: res_all[tp].astype(f32) + total,
        send_f,
        recv_f,
    )
    out[...] = out_all[...].reshape(rows, width)
    for c in started:
        c.wait_send()


NAMES = (
    "tokens",
    "g_mix",
    "w_query",
    "w_key",
    "w_value",
    "w_outgate",
    "w_decay",
    "cum_decay",
    "step_decay",
    "key_block",
    "value_block",
    "state",
    "g_heads",
    "w_out",
    "g_ffn",
    "w_gate",
    "w_up",
    "w_down",
)


def body(
    tokens,
    lengths,
    state,
    key_block,
    value_block,
    cum_decay,
    step_decay,
    g_mix,
    w_query,
    w_key,
    w_value,
    w_outgate,
    w_decay,
    g_heads,
    w_out,
    g_ffn,
    w_gate,
    w_up,
    w_down,
):
    n_kv = lax.axis_size("kv")
    n_tp = lax.axis_size("tp")
    rows, width = tokens.shape
    seqs = state.shape[0]
    units = w_gate.shape[1]
    piece = rows // n_tp
    arrays = dict(
        tokens=tokens,
        state=state,
        key_block=key_block,
        value_block=value_block,
        cum_decay=cum_decay,
        step_decay=step_decay,
        g_mix=g_mix.reshape(1, -1),
        w_query=w_query,
        w_key=w_key,
        w_value=w_value,
        w_outgate=w_outgate,
        w_decay=w_decay,
        g_heads=g_heads.reshape(1, -1),
        w_out=w_out,
        g_ffn=g_ffn.reshape(1, -1),
        w_gate=w_gate,
        w_up=w_up,
        w_down=w_down,
    )
    trees = tuple(RingTree(n_kv, h) for h in (HUBS_PROJ, HUBS_MIXED, HUBS_FFN, HUBS_HIDDEN))
    wide_a = 3 * DK + 2 * DV + LANES
    wide_d = 2 * (-(-(units + 1) // LANES) * LANES)
    dma = pltpu.SemaphoreType.DMA
    ring_sems = [dma((n_kv - 1,)), dma((n_kv - 1,))]
    tp_sems = [dma((2, n_tp)), dma((2, n_tp))]

    def stage_count(tree):
        return max(2 * (tree.levels() - 1), 1)

    scratch = [pltpu.VMEM(arrays[n].shape, arrays[n].dtype) for n in NAMES]
    scratch += [
        dma((len(NAMES),)),
        pltpu.VMEM((n_kv, seqs, wide_a), bf16),
        pltpu.VMEM((n_kv - 1, seqs, wide_a), bf16),
        pltpu.VMEM((stage_count(trees[0]), seqs, wide_a), bf16),
        pltpu.VMEM((n_kv, seqs, DV), bf16),
        pltpu.VMEM((n_tp, piece, width), bf16),
        pltpu.VMEM((n_tp, piece, width), bf16),
        pltpu.VMEM((n_tp, piece, width), bf16),
        pltpu.VMEM((n_kv, seqs, wide_d), bf16),
        pltpu.VMEM((n_kv - 1, seqs, wide_d), bf16),
        pltpu.VMEM((stage_count(trees[2]), seqs, wide_d), bf16),
        pltpu.VMEM((n_kv, seqs, units), bf16),
        pltpu.VMEM((n_tp, piece, width), bf16),
        pltpu.VMEM((n_tp, piece, width), bf16),
        pltpu.VMEM((n_tp, piece, width), bf16),
    ]
    scratch += ring_sems + ring_sems + tp_sems + ring_sems + ring_sems + tp_sems
    return pl.pallas_call(
        functools.partial(kernel, n_kv, n_tp, trees, NAMES),
        out_shape=jax.ShapeDtypeStruct((rows, width), bf16),
        in_specs=[pl.BlockSpec(memory_space=pltpu.MemorySpace.HBM)] * len(NAMES)
        + [pl.BlockSpec(memory_space=pltpu.MemorySpace.SMEM)],
        out_specs=pl.BlockSpec(memory_space=pltpu.MemorySpace.VMEM),
        scratch_shapes=scratch,
        compiler_params=pltpu.CompilerParams(
            collective_id=0, has_side_effects=True, vmem_limit_bytes=60 << 20
        ),
    )(*[arrays[n] for n in NAMES], lengths)


def solution(mesh):
    return jax.shard_map(
        body,
        mesh=mesh,
        in_specs=(
            P("grp", "kv"),
            P(("grp", "kv")),
            P(("grp", "kv"), "tp", None, None),
            P(("grp", "kv"), "tp", None, None),
            P(("grp", "kv"), "tp", None, None),
            P(("grp", "kv"), "tp", None, None),
            P(("grp", "kv"), "tp"),
            P("kv"),
            P("kv", "tp"),
            P("kv", "tp"),
            P("kv", "tp"),
            P("kv", "tp"),
            P("kv", "tp"),
            P("tp"),
            P("tp", "kv"),
            P("kv"),
            P("kv", "tp"),
            P("kv", "tp"),
            P("tp", "kv"),
        ),
        out_specs=P("grp", "kv"),
        check_vma=False,
    )
```
